32 devices in a mesh: sp: 8 (over z, core), tp: 4 (over y, x).
Axes of the slice: x: 2, y: 2, z: 4, core: 2. Of those that a mesh axis runs over, the one named last changes fastest.
Arguments:
- resid: bfloat16 [1536, 2048], P('sp', 'tp'), may hold values from -12 to 12
- conv_value: bfloat16 [1536, 2048], P('sp', 'tp'), may hold values from -80 to 80
- conv_gate: bfloat16 [1536, 2048], P('sp', 'tp'), may hold values from -6 to 6
- depth_kernel: float32 [31, 2048], P(None, 'tp'), may hold values from -1 to 1
- chan_gain: float32 [2048], P('tp'), may hold values from 0.1 to 1.9
- point_weight: bfloat16 [2048, 2048], P('tp'), may hold values from -0.125 to 0.125
- mix_gain: float32 [2048], replicated, may hold values from 0.1 to 1.9
- out_weight: bfloat16 [2048, 2048], P(None, 'tp'), may hold values from -0.125 to 0.125
- norm_gain: float32 [2048], P('tp'), may hold values from 0.1 to 1.9
- route_ids: int32 [1536, 4], P('sp'), may hold values from 0 to 31, all different within a row; in each aligned block of 192 rows (0 to 191, 192 to 383, ...) at most 32 rows name the same one
- route_weights: float32 [1536, 4], P('sp'), may hold values from 0.05 to 0.5
- gate_experts: bfloat16 [32, 2048, 4096], P('sp', None, 'tp'), may hold values from -0.3125 to 0.3125
- up_experts: bfloat16 [32, 2048, 4096], P('sp', None, 'tp'), may hold values from -0.3125 to 0.3125
- down_experts: bfloat16 [32, 4096, 2048], P('sp', 'tp'), may hold values from -0.09375 to 0.09375
Outputs:
- result: bfloat16 [1536, 2048], P('sp', 'tp')
The draws below stay inside these ranges and needn't reach their ends.
Inputs may be any that keep to these rules, and one draw needn't show every extreme that they name: `route_ids`: each row names 4 different experts; among the 192 rows of one index of sp no expert is named by more than 32 rows, and in some such block an expert is named by exactly 32.
All inputs are finite; a program needn't handle non-finite values.
Results may differ from the reference program's by a relative error of at most 0.024.
Values may be sent and summed in bfloat16 or wider, within the bound.
No kernel may reach another device: no remote copies, remote signals or barrier semaphores. Data moves between devices by JAX's collectives and lax.ppermute only.
A program may use at most 128 MiB of HBM per device.

```python
import math
import jax
import jax.numpy as jnp
import numpy as np
from jax import lax

D = 2048
CONV_CH = 2048
F = 4096
E = 32
TOPK = 4
WIDTH = 31
TOK_DEV = 192
TOKENS = 1536
CAP = 32
N_SP = 8
N_TP = 4


def scaled_draw(key, rows, columns, top):
    first, second = jax.random.split(key, 2)
    column_scale = top ** (jnp.arange(columns, dtype=jnp.float32) / columns)
    row_scale = jnp.exp(jax.random.uniform(second, (rows, 1), jnp.float32, -0.69, 0.69))
    base = jax.random.truncated_normal(first, -4.0, 4.0, (rows, columns), jnp.float32)
    return base * column_scale * row_scale


def draw_resid(key, part):
    values = scaled_draw(jax.random.fold_in(key, 11), TOKENS, D, 3.0) * 0.5
    return values.astype(jnp.bfloat16)


def draw_conv_value(key, part):
    values = scaled_draw(jax.random.fold_in(key, 23), TOKENS, CONV_CH, 10.0)
    return values.astype(jnp.bfloat16)


def levels(stream_key, dims, shards, least, high):
    level, own = 1.0, jax.random.fold_in(stream_key, 6)
    for dim, shards_of in shards:
        heights = jnp.exp(jax.random.uniform(jax.random.fold_in(own, dim), (shards_of,), jnp.float32, least / len(shards), high / len(shards)))
        level = level * jnp.repeat(heights, dims[dim] // shards_of).reshape([-1 if axis == dim else 1 for axis in range(len(dims))])
    return level


def assign_block(stream_key, own, number, rows, amount, top, reach, skew):
    order = jax.random.permutation(stream_key, amount)
    crowded, usual = load_shares(amount, rows * top, reach, skew, True), load_shares(amount, rows * top, reach, skew, False)
    places = jnp.arange(amount)

    def named(lengths, turn):
        used = int((lengths > 0).sum())
        fixed = max(1, used // 4)
        shifted = fixed + (places - fixed + turn * (used - fixed)) % max(1, amount - fixed)
        return jnp.zeros((amount,), jnp.int32).at[order[jnp.where(places < fixed, places, shifted)]].set(jnp.asarray(lengths, jnp.int32))

    lengths = jnp.where(number % 4 == 0, named(crowded, number // 4), named(usual, number - number // 4 - 1))
    mixed = jax.random.permutation(jax.random.fold_in(own, 3), amount)
    source_of, receiver = mixed[0:amount // 2 * 2:2], mixed[1:amount // 2 * 2:2]
    margin = jnp.minimum(lengths[source_of] - 1, reach - lengths[receiver]) // 2
    margin = jnp.where((source_of == order[0]) | (receiver == order[0]) | (lengths[receiver] == 0), 0, jnp.maximum(margin, 0))
    shifted = jax.random.randint(jax.random.fold_in(own, 4), (amount // 2,), 0, 1 << 20) % (margin + 1)
    lengths = lengths.at[source_of].add(-shifted).at[receiver].add(shifted)
    members = jnp.searchsorted(jnp.cumsum(lengths), jnp.arange(rows * top), side="right").astype(jnp.int32)
    grid = members.reshape(top, rows).T
    grid = grid[jax.random.permutation(jax.random.fold_in(own, 1), rows)]
    turn = jax.random.randint(jax.random.fold_in(own, 2), (rows, 1), 0, top)
    return jnp.take_along_axis(grid, (jnp.arange(top)[None, :] + turn) % top, axis=1)


def load_shares(amount, total, bound, slope, full):
    weights = [(1 << 20) // math.isqrt(standing ** slope) + 1 for standing in range(1, amount + 1)]
    largest = bound if full else min(bound, max(-(-total // amount), total * weights[0] // sum(weights)))
    least = 1 if total - largest >= amount - 1 else 0
    holding, spare = [largest] + [least] * (amount - 1), total - largest - least * (amount - 1)
    while spare > 0:
        movable = [i for i in range(1, amount) if holding[i] < largest] or [i for i in range(1, amount) if holding[i] < bound]
        pool, left = sum([weights[i] for i in movable]), spare
        for i in movable:
            addition = min(bound - holding[i], max(1, left * weights[i] // pool), spare)
            holding[i] = holding[i] + addition
            spare = spare - addition
    return np.array(holding)


def gaussian(key, extent, scale, most, pieces=(), kind=jnp.bfloat16):
    array = jax.random.normal(key, extent, jnp.float32) * scale
    if len(pieces) > 0:
        array = levels(key, extent, pieces, -0.22, 0.18) * array
    return jnp.clip(array, min=-most, max=most).astype(kind)


def setup_inputs(seed: int = 0) -> dict:
    key_of = jax.random.split(jax.random.key(seed), 15)
    resid = draw_resid(jax.random.fold_in(key_of[14], 71), 0)
    conv_value = draw_conv_value(jax.random.fold_in(key_of[14], 71), 0)
    conv_gate = gaussian(key_of[2], (TOKENS, CONV_CH), 1.5, 6.0, ((0, 8), (1, 4)))
    depth_kernel = gaussian(key_of[3], (WIDTH, CONV_CH), WIDTH ** -0.5, 1.0, ((1, 4),), jnp.float32)
    chan_gain = jnp.clip(1.0 + 0.18 * jax.random.normal(key_of[4], (CONV_CH,), jnp.float32), 0.1, 1.9)
    point_weight = gaussian(key_of[5], (CONV_CH, CONV_CH), CONV_CH ** -0.5, 0.125, ((0, 4),))
    mix_gain = jnp.clip(1.0 + 0.18 * jax.random.normal(key_of[6], (CONV_CH,), jnp.float32), 0.1, 1.9)
    out_weight = gaussian(key_of[7], (CONV_CH, D), CONV_CH ** -0.5, 0.125, ((1, 4),))
    norm_gain = jnp.clip(1.0 + 0.18 * jax.random.normal(key_of[8], (D,), jnp.float32), 0.1, 1.9)
    route_ids_keys = jax.random.split(jax.random.fold_in(key_of[9], 1), TOKENS // TOK_DEV)
    route_ids_turns = jax.random.permutation(jax.random.fold_in(key_of[9], 3), TOKENS // TOK_DEV)
    route_ids = jax.vmap(lambda own, number: assign_block(jax.random.fold_in(key_of[9], 2), own, number, TOK_DEV, E, TOPK, CAP, 2))(route_ids_keys, route_ids_turns).reshape((TOKENS, TOPK))
    route_weights = jnp.clip(0.05 + 0.45 * jax.random.uniform(key_of[10], (TOKENS, TOPK), jnp.float32) ** levels(key_of[10], (TOKENS, TOPK), ((0, 8),), -0.2, 0.2), 0.05, 0.5)
    gate_experts = gaussian(key_of[11], (E, D, F), (D // 6) ** -0.5, 0.3125, ((0, 8), (2, 4)))
    up_experts = gaussian(key_of[12], (E, D, F), (D // 6) ** -0.5, 0.3125, ((0, 8), (2, 4)))
    down_experts = gaussian(key_of[13], (E, F, D), F ** -0.5, 0.09375, ((0, 8), (1, 4)))
    return dict(resid=resid, conv_value=conv_value, conv_gate=conv_gate, depth_kernel=depth_kernel, chan_gain=chan_gain, point_weight=point_weight, mix_gain=mix_gain, out_weight=out_weight, norm_gain=norm_gain, route_ids=route_ids, route_weights=route_weights, gate_experts=gate_experts, up_experts=up_experts, down_experts=down_experts)


epsilon = 1e-05
clamp_limit = 7.0
swish_slope = 1.702

def rounded_sum(left, right, blocks):
    inner = left.shape[1] // blocks
    total = jnp.zeros((left.shape[0], right.shape[1]), jnp.float32)
    for block in range(blocks):
        part = jnp.dot(left[:, block * inner:(block + 1) * inner], right[block * inner:(block + 1) * inner], preferred_element_type=jnp.float32)
        total = total + lax.optimization_barrier(part.astype(jnp.bfloat16)).astype(jnp.float32)
    return total

def reference(resid, conv_value, conv_gate, depth_kernel, chan_gain, point_weight, mix_gain, out_weight, norm_gain, route_ids, route_weights, gate_experts, up_experts, down_experts):
    gated = (conv_value.astype(jnp.float32) * jax.nn.sigmoid(conv_gate.astype(jnp.float32))).astype(jnp.bfloat16)
    padded = jnp.concatenate([jnp.zeros((WIDTH - 1, CONV_CH), jnp.bfloat16), gated], axis=0)
    conv = jnp.zeros((TOKENS, CONV_CH), jnp.float32)
    for tap in range(WIDTH):
        conv = conv + padded[tap:tap + TOKENS].astype(jnp.float32) * depth_kernel[tap]
    center = conv - lax.optimization_barrier(jnp.mean(conv, axis=1, keepdims=True))
    spread = lax.optimization_barrier(jnp.mean(center * center, axis=1, keepdims=True))
    act = jax.nn.silu(center * lax.rsqrt(spread + epsilon) * chan_gain).astype(jnp.bfloat16)
    point = rounded_sum(act, point_weight, N_TP)
    mixed = (point * lax.rsqrt(lax.optimization_barrier(jnp.mean(point * point, axis=1, keepdims=True)) + epsilon) * mix_gain).astype(jnp.bfloat16)
    middle = (resid.astype(jnp.float32) + jnp.dot(mixed, out_weight, preferred_element_type=jnp.float32)).astype(jnp.bfloat16)
    middle32 = middle.astype(jnp.float32)
    normed = (middle32 * lax.rsqrt(lax.optimization_barrier(jnp.mean(middle32 * middle32, axis=1, keepdims=True)) + epsilon) * norm_gain).astype(jnp.bfloat16)
    flat_ids = route_ids.reshape(-1).astype(jnp.int32)
    flat_weights = route_weights.reshape(-1)
    routed = TOKENS * TOPK
    total = jnp.zeros((TOKENS, D), jnp.float32)
    for expert in range(E):
        found = jnp.nonzero(flat_ids == expert, size=N_SP * CAP, fill_value=routed)[0].astype(jnp.int32)
        valid = found < routed
        token = jnp.minimum(found // TOPK, TOKENS - 1).astype(jnp.int32)
        weight = jnp.where(valid, flat_weights[jnp.minimum(found, routed - 1)], 0.0)
        rows = normed[token]
        gate_pre = jnp.minimum(jnp.dot(rows, gate_experts[expert], preferred_element_type=jnp.float32), clamp_limit)
        up_pre = jnp.clip(jnp.dot(rows, up_experts[expert], preferred_element_type=jnp.float32), -clamp_limit, clamp_limit)
        hidden = (gate_pre * jax.nn.sigmoid(swish_slope * gate_pre) * (up_pre + 1.0)).astype(jnp.bfloat16)
        expert_out = rounded_sum(hidden, down_experts[expert], N_TP).astype(jnp.bfloat16)
        total = total.at[token].add(expert_out.astype(jnp.float32) * weight[:, None])
    return (middle32 + total).astype(jnp.bfloat16)
```

```python
import jax
import jax.numpy as jnp
from jax import lax
from jax.sharding import PartitionSpec as P


E = 32
TOPK = 4
CAP = 32


epsilon = 1e-05
clamp_limit = 7.0
swish_slope = 1.702

f32 = jnp.float32
bf16 = jnp.bfloat16


def from_behind(block, axis, distance):
    devices = range(lax.axis_size(axis))
    route = [(i - distance, i) for i in devices if i - distance in devices]
    return lax.ppermute(block, axis, route)


def swap(block, axis, bits):
    return lax.ppermute(block, axis, [(i, i ^ bits) for i in range(lax.axis_size(axis))])


def sum_tp(x):
    if lax.axis_size("tp") != 4:
        return lax.psum(x, "tp")
    return (x + swap(x, "tp", 1)) + (swap(x, "tp", 2) + swap(x, "tp", 3))


def scatter_rows_tp(x):
    tp = lax.axis_size("tp")
    if tp != 4:
        return lax.psum_scatter(x, "tp", scatter_dimension=0, tiled=True).astype(f32)
    me = lax.axis_index("tp")
    rows = x.shape[0] // tp
    block = lambda e: lax.dynamic_slice_in_dim(x, (me ^ e) * rows, rows, 0)
    arrived = [swap(block(e), "tp", e).astype(f32) for e in (3, 1, 2)]
    return block(0).astype(f32) + arrived[0] + arrived[1] + arrived[2]


def gather_rows_tp(x):
    tp = lax.axis_size("tp")
    if tp != 4:
        return lax.all_gather(x, "tp", axis=0, tiled=True)
    me = lax.axis_index("tp")
    rows = x.shape[0]
    out = jnp.zeros((tp * rows, x.shape[1]), x.dtype)
    for e, part in [(0, x)] + [(e, swap(x, "tp", e)) for e in (3, 1, 2)]:
        out = lax.dynamic_update_slice_in_dim(out, part, (me ^ e) * rows, 0)
    return out


def fast_mesh():
    return lax.axis_size("tp") == 4 and lax.axis_size("sp") == 8


def gather_meta(x):
    if not fast_mesh():
        return lax.all_gather(x, "sp")
    own = jnp.stack([x] + [swap(x, "sp", 2 * d) for d in (1, 2, 3)])
    other = swap(own, "sp", 1)
    return jnp.stack([own, other], axis=1).reshape((8,) + x.shape)


def gather_group(own):
    half = own.shape[1] // 2
    by_x = swap(own, "tp", 1)
    by_y = swap(own, "tp", 2)
    first = swap(by_x[:, :half], "tp", 2)
    second = swap(by_y[:, half:], "tp", 1)
    opposite = jnp.concatenate([first, second], axis=1)
    out = []
    for part in (own, by_x, by_y, opposite):
        out.append(jnp.stack([part, swap(part, "sp", 1)], axis=1))
    return out


def gather_tokens(x):
    rows, feats = x.shape
    if not fast_mesh():
        return lax.all_gather(lax.all_gather(x, "tp", axis=1, tiled=True), "sp")
    me = lax.axis_index("tp")
    groups = []
    near = jnp.stack([x, swap(x, "sp", 2)])
    far = jnp.stack([swap(x, "sp", 4), swap(x, "sp", 6)])
    for own in (near, far):
        parts = jnp.stack(gather_group(own))
        ordered = [lax.dynamic_index_in_dim(parts, me ^ a, 0, False) for a in range(4)]
        groups.append(jnp.concatenate(ordered, axis=-1).reshape(4, rows, 4 * feats))
    return groups


def scatter_group(partial):
    me = lax.axis_index("tp")
    rows = partial.shape[2]
    feats = partial.shape[3] // 4
    half = rows // 2
    cut = lambda a, e: lax.dynamic_slice_in_dim(a, (me ^ e) * feats, feats, 2)
    mine, other = partial[:, 0], partial[:, 1]
    block = {}
    for e in (3, 1, 2, 0):
        block[e] = cut(mine, e).astype(f32) + swap(cut(other, e), "sp", 1).astype(f32)
    far = block[3].astype(bf16)
    from_x = swap(far[:, :half], "tp", 1).astype(f32)
    from_y = swap(far[:, half:], "tp", 2).astype(f32)
    to_x = jnp.concatenate([block[1][:, :half], block[1][:, half:] + from_y], axis=1).astype(bf16)
    to_y = jnp.concatenate([block[2][:, :half] + from_x, block[2][:, half:]], axis=1).astype(bf16)
    return block[0] + swap(to_x, "tp", 1).astype(f32) + swap(to_y, "tp", 2).astype(f32)


def shards(
    resid,
    conv_value,
    conv_gate,
    depth_kernel,
    chan_gain,
    point_weight,
    mix_gain,
    out_weight,
    norm_gain,
    route_ids,
    route_weights,
    gate_experts,
    up_experts,
    down_experts,
):
    tok_rows, chan_local = conv_value.shape
    feat_local = resid.shape[1]
    local_experts = gate_experts.shape[0]
    slots = local_experts * CAP
    sources = lax.axis_size("sp")
    lookback = depth_kernel.shape[0] - 1

    flat_ids = route_ids.reshape(-1)
    expert_table = (flat_ids[:, None] == jnp.arange(E, dtype=jnp.int32)[None, :]).astype(jnp.int32)
    earlier_count = jnp.cumsum(expert_table, axis=0) - expert_table
    position = jnp.sum(earlier_count * expert_table, axis=1)
    slot_of = (flat_ids * CAP + position).reshape(tok_rows, TOPK)
    meta = gather_meta(jnp.concatenate([slot_of.astype(f32).T, route_weights.T], axis=0))
    slot_here = meta[:, :TOPK] - (lax.axis_index("sp") * slots).astype(f32)
    weight_here = meta[:, TOPK:]
    slot_ids = jnp.arange(slots, dtype=jnp.int32).astype(f32)

    gated = (conv_value.astype(f32) * jax.nn.sigmoid(conv_gate.astype(f32))).astype(bf16)
    earlier = from_behind(gated[tok_rows - lookback :], "sp", 1)
    padded = jnp.concatenate([earlier, gated], axis=0)
    conv = jnp.zeros((tok_rows, chan_local), f32)
    for tap in range(lookback + 1):
        conv = conv + padded[tap : tap + tok_rows].astype(f32) * depth_kernel[tap]
    chan_total = chan_local * lax.axis_size("tp")
    block_mean = jnp.mean(conv, axis=1)
    off = conv - block_mean[:, None]
    block_square = jnp.sum(off * off, axis=1)
    if lax.axis_size("tp") == 4:
        stats = jnp.stack([block_mean, block_square])
        every = [stats] + [swap(stats, "tp", e) for e in (3, 1, 2)]
        row_mean = sum(s[0] for s in every) / len(every)
        row_square = sum(s[1] + chan_local * jnp.square(s[0] - row_mean) for s in every)
    else:
        row_mean = lax.pmean(block_mean, "tp")
        row_square = lax.psum(block_square + chan_local * jnp.square(block_mean - row_mean), "tp")
    row_var = row_square / chan_total
    act = jax.nn.silu(
        (conv - row_mean[:, None]) * lax.rsqrt(row_var[:, None] + epsilon) * chan_gain
    ).astype(bf16)
    point = scatter_rows_tp(jnp.dot(act, point_weight, preferred_element_type=f32).astype(bf16))
    mixed = (
        point * lax.rsqrt(jnp.mean(point * point, axis=1, keepdims=True) + epsilon) * mix_gain
    ).astype(bf16)
    branch = jnp.dot(gather_rows_tp(mixed), out_weight, preferred_element_type=f32)
    middle = (resid.astype(f32) + branch).astype(bf16)
    middle32 = middle.astype(f32)
    feat_total = feat_local * lax.axis_size("tp")
    squares = sum_tp(jnp.sum(middle32 * middle32, axis=1))
    normed = (middle32 * lax.rsqrt(squares[:, None] / feat_total + epsilon) * norm_gain).astype(
        bf16
    )

    match = slot_here[:, :, None, :] == slot_ids[None, None, :, None]
    picker = jnp.any(match, axis=1).astype(bf16)
    spread = jnp.sum(jnp.where(match, weight_here[:, :, None, :], 0.0), axis=1).astype(bf16)
    tokens = gather_tokens(normed)
    if fast_mesh():
        per = sources // 2
        rows = jnp.concatenate(
            [
                jnp.einsum(
                    "sct,std->scd", picker[i * per : (i + 1) * per], part, preferred_element_type=f32
                ).astype(bf16)
                for i, part in enumerate(tokens)
            ]
        )
    else:
        rows = jnp.einsum("sct,std->scd", picker, tokens, preferred_element_type=f32).astype(bf16)
    rows = rows.reshape(sources, local_experts, CAP, rows.shape[2])
    gate_pre = jnp.minimum(
        jnp.einsum("sjcd,jdf->sjcf", rows, gate_experts, preferred_element_type=f32),
        clamp_limit,
    )
    up_pre = jnp.clip(
        jnp.einsum("sjcd,jdf->sjcf", rows, up_experts, preferred_element_type=f32),
        -clamp_limit,
        clamp_limit,
    )
    hidden = (gate_pre * jax.nn.sigmoid(swish_slope * gate_pre) * (up_pre + 1.0)).astype(bf16)
    partial_value = (
        jnp.einsum("sjcf,jfd->sjcd", hidden, down_experts, preferred_element_type=f32)
        .astype(bf16)
        .reshape(sources, slots, rows.shape[3])
    )

    def weigh(lo, hi):
        return jnp.einsum(
            "sct,scd->std", spread[lo:hi], partial_value[lo:hi], preferred_element_type=f32
        ).astype(bf16)

    if fast_mesh():
        per = sources // 2
        far = scatter_group(weigh(per, sources).reshape(2, 2, tok_rows, -1)).astype(bf16)
        far2 = swap(far[0], "sp", 4)
        far3 = swap(far[1], "sp", 6)
        near = scatter_group(weigh(0, per).reshape(2, 2, tok_rows, -1))
        near1 = swap(near[1].astype(bf16), "sp", 2)
        routed_sum = near[0] + near1.astype(f32) + far2.astype(f32) + far3.astype(f32)
    else:
        sums = lax.psum_scatter(weigh(0, sources), "tp", scatter_dimension=2, tiled=True)
        routed_sum = lax.psum_scatter(sums, "sp").astype(f32)
    return (middle32 + routed_sum).astype(bf16)


def solution(mesh):
    in_specs = (
        P("sp", "tp"),
        P("sp", "tp"),
        P("sp", "tp"),
        P(None, "tp"),
        P("tp"),
        P("tp", None),
        P(),
        P(None, "tp"),
        P("tp"),
        P("sp", None),
        P("sp", None),
        P("sp", None, "tp"),
        P("sp", None, "tp"),
        P("sp", "tp", None),
    )
    out_specs = P("sp", "tp")
    return jax.shard_map(shards, mesh=mesh, in_specs=in_specs, out_specs=out_specs, check_vma=False)
```
